32 devices in a mesh: fs: 8 (over z, x), tp: 4 (over y, core).
Axes of the slice: x: 2, y: 2, z: 4, core: 2. Of those that a mesh axis runs over, the one named last changes fastest.
Arguments:
- tokens: bfloat16 [8192, 2048], P('fs'), may hold values from -3 to 3
- gate_weight: bfloat16 [2048, 5632], P('fs', 'tp'), may hold values from -0.125 to 0.125
- value_weight: bfloat16 [2048, 5632], P('fs', 'tp'), may hold values from -0.125 to 0.125
- gate_taps: bfloat16 [3, 5632], P(None, 'tp'), may hold values from -3 to 3
- value_taps: bfloat16 [3, 5632], P(None, 'tp'), may hold values from -3 to 3
- down_weight: bfloat16 [5632, 2048], P('tp', 'fs'), may hold values from -0.078125 to 0.078125
- norm_gain: float32 [2048], replicated, may hold values from 0.1 to 1.9
- norm_bias: float32 [2048], replicated, may hold values from -3 to 3
Outputs:
- normed: bfloat16 [8192, 2048], P('fs')
The draws below stay inside these ranges and needn't reach their ends.
All inputs are finite; a program needn't handle non-finite values.
Results may differ from the reference program's by a relative error of at most 0.005.
Values may be sent and summed in bfloat16 or wider, within the bound.
No kernel may reach another device: no remote copies, remote signals or barrier semaphores. Data moves between devices by JAX's collectives and lax.ppermute only.
A program may use at most 64 MiB of HBM per device.

```python
import jax
import jax.numpy as jnp
from jax import lax

D = 2048
FF = 5632
TOK_DEV = 1024
TOKENS = 8192
N_FS = 8
N_TP = 4


def block_scale(rng, dims, shards, least, high):
    def one(position, blocks):
        heights = jax.random.uniform(jax.random.fold_in(jax.random.fold_in(rng, 6), position), (blocks,), jnp.float32, least / len(shards), high / len(shards))
        return jnp.repeat(jnp.exp(heights), dims[position] // blocks).reshape((-1,) + (1,) * (len(dims) - position - 1))

    factor_of = one(*shards[0])
    for cut in shards[1:]:
        factor_of = factor_of * one(*cut)
    return factor_of


def scatter_about(key, dims, deviation, limit, pieces=(), held_as=jnp.bfloat16):
    result = jax.random.normal(key, dims, jnp.float32) * deviation
    if len(pieces) > 0:
        result = block_scale(key, dims, pieces, -0.22, 0.18) * result
    return jnp.clip(result, min=-limit, max=limit).astype(held_as)


def setup_inputs(seed: int = 0) -> dict:
    streams_of = jax.random.split(jax.random.key(seed), 9)
    return {
        "tokens": scatter_about(streams_of[0], (TOKENS, D), 0.5, 3.0, ((0, 8),)),
        "gate_weight": scatter_about(streams_of[1], (D, FF), D ** -0.5, 0.125, ((0, 8), (1, 4))),
        "value_weight": scatter_about(streams_of[2], (D, FF), D ** -0.5, 0.125, ((0, 8), (1, 4))),
        "gate_taps": scatter_about(streams_of[3], (3, FF), 0.577, 3.0, ((1, 4),)),
        "value_taps": scatter_about(streams_of[4], (3, FF), 0.577, 3.0, ((1, 4),)),
        "down_weight": scatter_about(streams_of[5], (FF, D), FF ** -0.5, 0.078125, ((0, 4), (1, 8))),
        "norm_gain": jnp.clip(1.0 + 0.18 * jax.random.normal(streams_of[6], (D,), jnp.float32), 0.1, 1.9),
        "norm_bias": scatter_about(streams_of[7], (D,), 0.5, 3.0, (), jnp.float32),
    }


EPSILON = 1e-05
RESIDUAL_SCALE = 8.0 ** 0.25

def rounded(values):
    return lax.optimization_barrier(values.astype(jnp.bfloat16)).astype(jnp.float32)

def centred_conv(values, taps):
    padded = jnp.pad(values, ((0, 0), (1, 1), (0, 0)))
    return padded[:, :-2] * taps[0] + padded[:, 1:-1] * taps[1] + padded[:, 2:] * taps[2]

def reference(tokens, gate_weight, value_weight, gate_taps, value_taps, down_weight, norm_gain, norm_bias):
    gate_lin = rounded(jnp.dot(tokens, gate_weight, preferred_element_type=jnp.float32))
    value_lin = rounded(jnp.dot(tokens, value_weight, preferred_element_type=jnp.float32))
    layout = (N_FS, TOK_DEV, FF)
    gate_conv = centred_conv(gate_lin.reshape(layout), gate_taps.astype(jnp.float32))
    value_conv = centred_conv(value_lin.reshape(layout), value_taps.astype(jnp.float32))
    hidden = (jax.nn.silu(gate_conv) * value_conv).astype(jnp.bfloat16).reshape(TOKENS, FF)
    block_width = FF // N_TP

    def add_block(summed, index):
        columns = lax.dynamic_slice_in_dim(hidden, index * block_width, block_width, 1)
        weight_rows = lax.dynamic_slice_in_dim(down_weight, index * block_width, block_width, 0)
        partial_value = jnp.dot(columns, weight_rows, preferred_element_type=jnp.float32)
        return (summed + rounded(partial_value), None)
    summed, _ = lax.scan(add_block, jnp.zeros((TOKENS, D), jnp.float32), jnp.arange(N_TP, dtype=jnp.int32))
    mixed = RESIDUAL_SCALE * tokens.astype(jnp.float32) + rounded(summed)
    centered = mixed - lax.optimization_barrier(jnp.mean(mixed, -1, keepdims=True))
    variance = lax.optimization_barrier(jnp.mean(centered * centered, -1, keepdims=True))
    normed = centered * lax.rsqrt(variance + EPSILON) * norm_gain + norm_bias
    return normed.astype(jnp.bfloat16)
```

```python
import jax
import jax.numpy as jnp
from jax import lax
from jax.sharding import PartitionSpec as P

EPSILON = 1e-05
RESIDUAL_SCALE = 8.0**0.25
CORES = 2


def centred_conv(values, taps):
    padded = jnp.pad(values, ((1, 1), (0, 0)))
    return padded[:-2] * taps[0] + padded[1:-1] * taps[1] + padded[2:] * taps[2]


def grid_of(mesh):
    coords = [d.coords for d in mesh.devices[:, 0]]
    n_x = len({c[0] for c in coords})
    return len(coords) // n_x, n_x


def solution(mesh):
    n_z, n_x = grid_of(mesh)
    n_fs, n_tp = mesh.shape["fs"], mesh.shape["tp"]
    n_y = n_tp // CORES
    z_next = [(((z + 1) % n_z) * n_x + x, z * n_x + x) for z in range(n_z) for x in range(n_x)]
    x_next = [(z * n_x + (x + 1) % n_x, z * n_x + x) for z in range(n_z) for x in range(n_x)]
    core_swap = [(t, t ^ 1) for t in range(n_tp)]
    y_next = [(((y + 1) % n_y) * CORES + c, y * CORES + c) for y in range(n_y) for c in range(CORES)]

    def gather(own, x_first):
        index = lax.axis_index("fs")
        z, x = index // n_x, index % n_x
        found = []

        def x_ring(piece, dz):
            for dx in range(1, n_x):
                piece = lax.ppermute(piece, "fs", x_next)
                yield dx, piece

        def where(dz, dx):
            return ((z + dz) % n_z) * n_x + (x + dx) % n_x

        if x_first:
            columns = [(0, own)] + list(x_ring(own, 0))
            for dx, piece in columns:
                found.append((where(0, dx), piece))
            for dz in range(1, n_z):
                columns = [(dx, lax.ppermute(piece, "fs", z_next)) for dx, piece in columns]
                for dx, piece in columns:
                    found.append((where(dz, dx), piece))
        else:
            piece = own
            for dz in range(n_z):
                if dz:
                    piece = lax.ppermute(piece, "fs", z_next)
                found.append((where(dz, 0), piece))
                for dx, other in x_ring(piece, dz):
                    found.append((where(dz, dx), other))
        return found

    def on_device(tokens, gate_weight, value_weight, gate_taps, value_taps, down_weight, norm_gain, norm_bias):
        rows, width = tokens.shape
        shard = gate_weight.shape[0]
        core = lax.axis_index("tp") % CORES
        half = rows // CORES

        def whole(own):
            full = jnp.zeros((width, own.shape[1]), own.dtype)
            for index, piece in gather(own, False):
                full = lax.dynamic_update_slice_in_dim(full, piece, index * shard, 0)
            return full

        def up(own):
            return jnp.dot(tokens, whole(own), preferred_element_type=jnp.float32).astype(jnp.bfloat16)

        gate_lin = up(gate_weight)
        value_lin = up(value_weight)
        gate_conv = centred_conv(gate_lin.astype(jnp.float32), gate_taps.astype(jnp.float32))
        value_conv = centred_conv(value_lin.astype(jnp.float32), value_taps.astype(jnp.float32))
        hidden = (jax.nn.silu(gate_conv) * value_conv).astype(jnp.bfloat16)
        kept = lax.dynamic_slice_in_dim(hidden, core * half, half, 0)
        given = lax.dynamic_slice_in_dim(hidden, (CORES - 1 - core) * half, half, 0)

        cols = down_weight.shape[1]
        part = cols // 2
        branch = jnp.zeros((half, width), jnp.bfloat16)
        pieces = []
        first = gather(down_weight[:, :part], True)
        second = gather(down_weight[:, part:], False)
        for (i, a), (j, b) in zip(first, second):
            pieces += [(i * cols, a), (j * cols + part, b)]
        for column, weight in pieces:
            sent = jnp.dot(given, weight, preferred_element_type=jnp.float32).astype(jnp.bfloat16)
            mine = jnp.dot(kept, weight, preferred_element_type=jnp.float32)
            chip = mine + lax.ppermute(sent, "tp", core_swap).astype(jnp.float32)
            moving = chip.astype(jnp.bfloat16)
            total = moving.astype(jnp.float32)
            for _ in range(1, n_y):
                moving = lax.ppermute(moving, "tp", y_next)
                total = total + moving.astype(jnp.float32)
            branch = lax.dynamic_update_slice_in_dim(branch, total.astype(jnp.bfloat16), column, 1)

        own_rows = lax.dynamic_slice_in_dim(tokens, core * half, half, 0)
        mixed = RESIDUAL_SCALE * own_rows.astype(jnp.float32) + branch.astype(jnp.float32)
        centered = mixed - jnp.mean(mixed, -1, keepdims=True)
        variance = jnp.mean(centered * centered, -1, keepdims=True)
        normed = (centered * lax.rsqrt(variance + EPSILON) * norm_gain + norm_bias).astype(jnp.bfloat16)
        other = lax.ppermute(normed, "tp", core_swap)
        out = jnp.zeros((rows, width), jnp.bfloat16)
        out = lax.dynamic_update_slice_in_dim(out, normed, core * half, 0)
        return lax.dynamic_update_slice_in_dim(out, other, (CORES - 1 - core) * half, 0)

    in_specs = (
        P("fs", None),
        P("fs", "tp"),
        P("fs", "tp"),
        P(None, "tp"),
        P(None, "tp"),
        P("tp", "fs"),
        P(),
        P(),
    )
    return jax.shard_map(on_device, mesh=mesh, in_specs=in_specs, out_specs=P("fs", None), check_vma=False)
```

```python
import jax
import jax.numpy as jnp
from jax import lax
from jax.sharding import PartitionSpec as P


EPSILON = 1e-05
RESIDUAL_SCALE = 8.0**0.25
CORES = 2


def centred_conv(values, taps):
    padded = jnp.pad(values, ((1, 1), (0, 0)))
    return padded[:-2] * taps[0] + padded[1:-1] * taps[1] + padded[2:] * taps[2]


def grid_of(mesh):
    coords = [d.coords for d in mesh.devices[:, 0]]
    n_x = len({c[0] for c in coords})
    return len(coords) // n_x, n_x


def solution(mesh):
    n_z, n_x = grid_of(mesh)
    n_tp = mesh.shape["tp"]
    n_y = n_tp // CORES

    def z_shift(d):
        return [(((z + d) % n_z) * n_x + x, z * n_x + x) for z in range(n_z) for x in range(n_x)]

    x_next = [(z * n_x + (x + 1) % n_x, z * n_x + x) for z in range(n_z) for x in range(n_x)]
    core_swap = [(t, t ^ 1) for t in range(n_tp)]
    y_next = [(((y + 1) % n_y) * CORES + c, y * CORES + c) for y in range(n_y) for c in range(CORES)]

    def after(value, *others):
        return lax.optimization_barrier((value, *others))[0]

    def on_device(tokens, gate_weight, value_weight, gate_taps, value_taps, down_weight, norm_gain, norm_bias):
        rows, width = tokens.shape
        shard = gate_weight.shape[0]
        core = lax.axis_index("tp") % CORES
        half = rows // CORES

        index = lax.axis_index("fs")
        z, x = index // n_x, index % n_x
        order = [0] + sorted(range(1, n_z), key=lambda d: (min(d, n_z - d), d))

        def where(dz, dx):
            return ((z + dz) % n_z) * n_x + (x + dx) % n_x

        def up(rows_of, *before):
            full = jnp.zeros((width, gate_weight.shape[1]), gate_weight.dtype)
            for dz in order:
                for dx, piece in enumerate(rows_of[dz]):
                    if dz == order[-1] and before:
                        piece = after(piece, *before)
                    full = lax.dynamic_update_slice_in_dim(full, piece, where(dz, dx) * shard, 0)
            return jnp.dot(tokens, full, preferred_element_type=jnp.float32).astype(jnp.bfloat16)

        def z_send(found, dz):
            if dz <= n_z // 2:
                found[dz] = lax.ppermute(found[dz - 1], "fs", z_shift(1))
            else:
                found[dz] = lax.ppermute(found[(dz + 1) % n_z], "fs", z_shift(-1))

        def x_ring(own):
            found = [own]
            for _ in range(1, n_x):
                found.append(lax.ppermute(found[-1], "fs", x_next))
            return found

        cols = down_weight.shape[1]
        part = cols // 2
        near = order[1:3]
        far = order[3:]
        gate_found, value_found = {0: gate_weight}, {0: value_weight}
        gate_rows, value_rows = {}, {}
        late_found = {0: down_weight[:, part:]}
        late_columns = {}
        for found, rows_of in ((gate_found, gate_rows), (value_found, value_rows)):
            for dz in near:
                z_send(found, dz)
            rows_of[0] = x_ring(found[0])
        early_found = [{0: piece} for piece in x_ring(down_weight[:, :part])]
        late_columns[0] = x_ring(late_found[0])
        for found, rows_of in ((gate_found, gate_rows), (value_found, value_rows)):
            for n, dz in enumerate(near):
                if n < len(far):
                    z_send(found, far[n])
                rows_of[dz] = x_ring(found[dz])
        for found, rows_of in ((gate_found, gate_rows), (value_found, value_rows)):
            for n, dz in enumerate(far):
                if n + 2 < len(far):
                    z_send(found, far[n + 2])
                rows_of[dz] = x_ring(found[dz])
        for dz in near:
            for found in (*early_found, late_found):
                z_send(found, dz)
        gate_lin = up(gate_rows)
        for found in (*early_found, late_found):
            for dz in near:
                found[dz] = after(found[dz], gate_lin)
        for dz in far:
            for found in (*early_found, late_found):
                z_send(found, dz)
        for dz in near:
            late_columns[dz] = x_ring(late_found[dz])
        value_lin = up(value_rows, gate_lin)
        gate_conv = centred_conv(gate_lin.astype(jnp.float32), gate_taps.astype(jnp.float32))
        value_conv = centred_conv(value_lin.astype(jnp.float32), value_taps.astype(jnp.float32))
        hidden = (jax.nn.silu(gate_conv) * value_conv).astype(jnp.bfloat16)
        kept = lax.dynamic_slice_in_dim(hidden, core * half, half, 0)
        given = lax.dynamic_slice_in_dim(hidden, (CORES - 1 - core) * half, half, 0)

        branch = jnp.zeros((half, width), jnp.bfloat16)
        for dz in order:
            if dz == near[0]:
                for other in far:
                    late_columns[other] = x_ring(late_found[other])
            group = [(where(dz, dx) * cols, found[dz]) for dx, found in enumerate(early_found)]
            group += [(where(dz, dx) * cols + part, piece) for dx, piece in enumerate(late_columns[dz])]
            if dz in far:
                group = [(column, after(piece, hidden)) for column, piece in group]
            weight = jnp.concatenate([piece for _, piece in group], 1)
            sent = jnp.dot(given, weight, preferred_element_type=jnp.float32).astype(jnp.bfloat16)
            mine = jnp.dot(kept, weight, preferred_element_type=jnp.float32)
            chip = mine + lax.ppermute(sent, "tp", core_swap).astype(jnp.float32)
            moving = chip.astype(jnp.bfloat16)
            total = moving.astype(jnp.float32)
            for _ in range(1, n_y):
                moving = lax.ppermute(moving, "tp", y_next)
                total = total + moving.astype(jnp.float32)
            total = total.astype(jnp.bfloat16)
            for k, (column, _) in enumerate(group):
                block = total[:, k * part : (k + 1) * part]
                branch = lax.dynamic_update_slice_in_dim(branch, block, column, 1)

        own_rows = lax.dynamic_slice_in_dim(tokens, core * half, half, 0)
        mixed = RESIDUAL_SCALE * own_rows.astype(jnp.float32) + branch.astype(jnp.float32)
        centered = mixed - jnp.mean(mixed, -1, keepdims=True)
        variance = jnp.mean(centered * centered, -1, keepdims=True)
        normed = (centered * lax.rsqrt(variance + EPSILON) * norm_gain + norm_bias).astype(jnp.bfloat16)
        other = lax.ppermute(normed, "tp", core_swap)
        out = jnp.zeros((rows, width), jnp.bfloat16)
        out = lax.dynamic_update_slice_in_dim(out, normed, core * half, 0)
        return lax.dynamic_update_slice_in_dim(out, other, (CORES - 1 - core) * half, 0)

    in_specs = (
        P("fs", None),
        P("fs", "tp"),
        P("fs", "tp"),
        P(None, "tp"),
        P(None, "tp"),
        P("tp", "fs"),
        P(),
        P(),
    )
    step = jax.shard_map(on_device, mesh=mesh, in_specs=in_specs, out_specs=P("fs", None), check_vma=False)

    def ordered(*args):
        jax.eval_shape(step, *args)
        return step(*args)

    return ordered
```
